32 devices in a mesh: ep: 8 (over z, y), tp: 4 (over x, core).
Axes of the slice: x: 2, y: 2, z: 4, core: 2. Of those that a mesh axis runs over, the one named last changes fastest.
Arguments:
- tokens: bfloat16 [384, 2048], P(('ep', 'tp')), may hold values from -6 to 6
- cache_latent: bfloat16 [384, 1024, 512], P(('ep', 'tp')), may hold values from -1700 to 1700
- cache_rope: bfloat16 [384, 64, 1024], P(('ep', 'tp')), may hold values from -6 to 6
- lengths: int32 [384], P(('ep', 'tp')), may hold values from 128 to 1023, as said below
- attn_gain: bfloat16 [2048], replicated, may hold values from 0.099609375 to 1.8984375
- latent_gain: bfloat16 [512], replicated, may hold values from 0.099609375 to 1.8984375
- post_attn_gain: bfloat16 [2048], replicated, may hold values from 0.099609375 to 1.8984375
- ffn_gain: bfloat16 [2048], replicated, may hold values from 0.099609375 to 1.8984375
- post_ffn_gain: bfloat16 [2048], replicated, may hold values from 0.099609375 to 1.8984375
- w_query: bfloat16 [2048, 2048], P(None, 'tp'), may hold values from -0.125 to 0.125
- w_query_rot: bfloat16 [2048, 1024], P(None, 'tp'), may hold values from -0.125 to 0.125
- w_latent: bfloat16 [2048, 512], P(None, 'tp'), may hold values from -0.125 to 0.125
- w_key_rot: bfloat16 [2048, 64], replicated, may hold values from -0.125 to 0.125
- w_key_up: bfloat16 [512, 16, 128], P(None, 'tp'), may hold values from -0.25 to 0.25
- w_value_up: bfloat16 [512, 16, 128], P(None, 'tp'), may hold values from -0.25 to 0.25
- w_out: bfloat16 [2048, 2048], P('tp'), may hold values from -0.125 to 0.125
- route_logits: float32 [384, 4], P('ep'), may hold values from -6 to 6
- routes: int32 [384, 4], P('ep'), may hold values from 0 to 7, all different within a row; in each aligned block of 48 rows (0 to 47, 48 to 95, ...) at most 25 rows name the same one
- w_gate: bfloat16 [8, 2048, 2048], P('ep', None, 'tp'), may hold values from -0.3125 to 0.3125
- w_up: bfloat16 [8, 2048, 2048], P('ep', None, 'tp'), may hold values from -0.3125 to 0.3125
- w_down: bfloat16 [8, 2048, 2048], P('ep', 'tp'), may hold values from -0.125 to 0.125
Outputs:
- result: bfloat16 [384, 2048], P(('ep', 'tp'))
- new_latent: bfloat16 [384, 512], P(('ep', 'tp'))
- new_rope: bfloat16 [384, 64], P(('ep', 'tp'))
The draws below stay inside these ranges and needn't reach their ends.
Inputs may be any that keep to these rules, and one draw needn't show every extreme that they name: Each sequence's cache holds positions 0 to lengths - 1, and the new token stands at position lengths; some sequence has 1023 in every draw. `routes`: each row names 4 different experts; in each aligned block of 48 rows (the tokens of one index of ep) no expert is named more than 25 times, a bound that some block reaches.
All inputs are finite; a program needn't handle non-finite values.
Results may differ from the reference program's by a relative error of at most 0.019.
Values may be sent and summed in bfloat16 or wider, within the bound.
A program may use at most 128 MiB of HBM per device.

```python
import math
import jax
import jax.numpy as jnp
import numpy as np
from jax import lax

D = 2048
HEADS = 16
KEY_DIM = 128
ROT_DIM = 64
VAL_DIM = 128
LATENT = 512
FF = 2048
TOP_K = 4
SEQ_DEV = 12
LEN = 1024
EXPERTS = 8
GROUP = 48
BATCH = 384
CAP = 25
N_TP = 4


def draw_cache_latent(key, part):
    base_key = jax.random.fold_in(jax.random.fold_in(key, 11), 0)
    cache = jnp.clip(jax.random.normal(base_key, (BATCH, LEN, LATENT), jnp.float32), -5.0, 5.0)
    return cache.astype(jnp.bfloat16)


def draw_lengths(key, part):
    keys = jax.random.split(jax.random.fold_in(key, 23), 3)
    lowest = LEN // 8
    ceilings = jax.random.randint(keys[0], (BATCH // SEQ_DEV,), LEN // 4, LEN)
    ceilings = jnp.repeat(ceilings, SEQ_DEV)
    drawn = jax.random.randint(keys[1], (BATCH,), lowest, ceilings)
    longest = jax.random.randint(keys[2], (), 0, BATCH)
    return jnp.where(jnp.arange(BATCH) == longest, LEN - 1, drawn).astype(jnp.int32)


def block_levels(rng, shape, cuts, least, top_value):
    def one(position, shards_of):
        heights = jax.random.uniform(jax.random.fold_in(jax.random.fold_in(rng, 6), position), (shards_of,), jnp.float32, least / len(cuts), top_value / len(cuts))
        return jnp.repeat(jnp.exp(heights), shape[position] // shards_of).reshape((-1,) + (1,) * (len(shape) - position - 1))

    loudness = one(*cuts[0])
    for cut in cuts[1:]:
        loudness = loudness * one(*cut)
    return loudness


def assign_block(stream_key, own, number, rows, count, top, limit, lean):
    order = jax.random.permutation(stream_key, count)
    heavy_load, ordinary = shares(count, rows * top, limit, lean, True), shares(count, rows * top, limit, lean, False)
    places = jnp.arange(count)

    def named(sizes, offset_by):
        used = int((sizes > 0).sum())
        fixed = max(1, used // 4)
        shifted = fixed + (places - fixed + offset_by * (used - fixed)) % max(1, count - fixed)
        return jnp.zeros((count,), jnp.int32).at[order[jnp.where(places < fixed, places, shifted)]].set(jnp.asarray(sizes, jnp.int32))

    sizes = jnp.where(number % 4 == 0, named(heavy_load, number // 4), named(ordinary, number - number // 4 - 1))
    mixed = jax.random.permutation(jax.random.fold_in(own, 3), count)
    source_of, sink = mixed[0:count // 2 * 2:2], mixed[1:count // 2 * 2:2]
    room = jnp.minimum(sizes[source_of] - 1, limit - sizes[sink]) // 2
    room = jnp.where((source_of == order[0]) | (sink == order[0]) | (sizes[sink] == 0), 0, jnp.maximum(room, 0))
    shifted = jax.random.randint(jax.random.fold_in(own, 4), (count // 2,), 0, 1 << 20) % (room + 1)
    sizes = sizes.at[source_of].add(-shifted).at[sink].add(shifted)
    members = jnp.searchsorted(jnp.cumsum(sizes), jnp.arange(rows * top), side="right").astype(jnp.int32)
    table = members.reshape(top, rows).T
    table = table[jax.random.permutation(jax.random.fold_in(own, 1), rows)]
    offset_by = jax.random.randint(jax.random.fold_in(own, 2), (rows, 1), 0, top)
    return jnp.take_along_axis(table, (jnp.arange(top)[None, :] + offset_by) % top, axis=1)


def shares(number_of, total, bound, slope, full):
    loads = [(1 << 20) // math.isqrt(grade ** slope) + 1 for grade in range(1, number_of + 1)]
    largest = bound if full else min(bound, max(-(-total // number_of), total * loads[0] // sum(loads)))
    least = 1 if total - largest >= number_of - 1 else 0
    given, rest = [largest] + [least] * (number_of - 1), total - largest - least * (number_of - 1)
    while rest > 0:
        free = [i for i in range(1, number_of) if given[i] < largest] or [i for i in range(1, number_of) if given[i] < bound]
        pool, budget = sum([loads[i] for i in free]), rest
        for i in free:
            addition = min(bound - given[i], max(1, budget * loads[i] // pool), rest)
            given[i] = given[i] + addition
            rest = rest - addition
    return np.array(given)


def bell_draw(key, shape, scale, most, cuts=(), kind=jnp.bfloat16):
    values = scale * jax.random.normal(key, shape, jnp.float32)
    if cuts:
        values = values * block_levels(key, shape, cuts, -0.22, 0.18)
    return jnp.clip(values, -most, most).astype(kind)


def setup_inputs(seed: int = 0) -> dict:
    key_list = jax.random.split(jax.random.key(seed), 22)
    tokens = bell_draw(key_list[0], (BATCH, D), 1.0, 6.0, ((0, 32),))
    cache_latent = draw_cache_latent(jax.random.fold_in(key_list[21], 71), 0)
    cache_rope = bell_draw(key_list[2], (BATCH, ROT_DIM, LEN), 1.0, 6.0, ((0, 32),))
    lengths = draw_lengths(jax.random.fold_in(key_list[21], 71), 0)
    attn_gain = jnp.clip(1.0 + 0.18 * jax.random.normal(key_list[4], (D,), jnp.float32), 0.099609375, 1.8984375).astype(jnp.bfloat16)
    latent_gain = jnp.clip(1.0 + 0.18 * jax.random.normal(key_list[5], (LATENT,), jnp.float32), 0.099609375, 1.8984375).astype(jnp.bfloat16)
    post_attn_gain = jnp.clip(1.0 + 0.18 * jax.random.normal(key_list[6], (D,), jnp.float32), 0.099609375, 1.8984375).astype(jnp.bfloat16)
    ffn_gain = jnp.clip(1.0 + 0.18 * jax.random.normal(key_list[7], (D,), jnp.float32), 0.099609375, 1.8984375).astype(jnp.bfloat16)
    post_ffn_gain = jnp.clip(1.0 + 0.18 * jax.random.normal(key_list[8], (D,), jnp.float32), 0.099609375, 1.8984375).astype(jnp.bfloat16)
    w_query = bell_draw(key_list[9], (D, HEADS * KEY_DIM), D ** -0.5, 0.125, ((1, 4),))
    w_query_rot = bell_draw(key_list[10], (D, HEADS * ROT_DIM), D ** -0.5, 0.125, ((1, 4),))
    w_latent = bell_draw(key_list[11], (D, LATENT), D ** -0.5, 0.125, ((1, 4),))
    w_key_rot = bell_draw(key_list[12], (D, ROT_DIM), D ** -0.5, 0.125)
    w_key_up = bell_draw(key_list[13], (LATENT, HEADS, KEY_DIM), LATENT ** -0.5, 0.25, ((1, 4),))
    w_value_up = bell_draw(key_list[14], (LATENT, HEADS, VAL_DIM), LATENT ** -0.5, 0.25, ((1, 4),))
    w_out = bell_draw(key_list[15], (HEADS * VAL_DIM, D), (HEADS * VAL_DIM) ** -0.5, 0.125, ((0, 4),))
    route_logits = bell_draw(key_list[16], (BATCH, TOP_K), 1.0, 6.0, ((0, 8),), jnp.float32)
    routes_keys = jax.random.split(jax.random.fold_in(key_list[17], 1), BATCH // GROUP)
    routes_turns = jax.random.permutation(jax.random.fold_in(key_list[17], 3), BATCH // GROUP)
    routes = jax.vmap(lambda own, number: assign_block(jax.random.fold_in(key_list[17], 2), own, number, GROUP, EXPERTS, TOP_K, CAP, 2))(routes_keys, routes_turns).reshape((BATCH, TOP_K))
    w_gate = bell_draw(key_list[18], (EXPERTS, D, FF), 0.055, 0.3125, ((0, 8), (2, 4)))
    w_up = bell_draw(key_list[19], (EXPERTS, D, FF), 0.055, 0.3125, ((0, 8), (2, 4)))
    w_down = bell_draw(key_list[20], (EXPERTS, FF, D), FF ** -0.5, 0.125, ((0, 8), (1, 4)))
    return dict(tokens=tokens, cache_latent=cache_latent, cache_rope=cache_rope, lengths=lengths, attn_gain=attn_gain, latent_gain=latent_gain, post_attn_gain=post_attn_gain, ffn_gain=ffn_gain, post_ffn_gain=post_ffn_gain, w_query=w_query, w_query_rot=w_query_rot, w_latent=w_latent, w_key_rot=w_key_rot, w_key_up=w_key_up, w_value_up=w_value_up, w_out=w_out, route_logits=route_logits, routes=routes, w_gate=w_gate, w_up=w_up, w_down=w_down)


eps_norm = 1e-06
clamp_limit = 7.0
sigmoid_alpha = 1.702
theta_base = 10000.0

def rms_scale(values, gain):
    mean_square = lax.optimization_barrier(jnp.mean(values * values, axis=-1, keepdims=True))
    return values * lax.rsqrt(mean_square + eps_norm) * gain.astype(jnp.float32)

def rotate(values, positions):
    half = values.shape[-1] // 2
    freqs = theta_base ** (-jnp.arange(half, dtype=jnp.float32) / half)
    angles = positions[..., None] * freqs
    cosine = jnp.cos(angles)
    sine = jnp.sin(angles)
    first = values[..., :half]
    second = values[..., half:]
    return jnp.concatenate([first * cosine - second * sine, second * cosine + first * sine], axis=-1)

def reference(tokens, cache_latent, cache_rope, lengths, attn_gain, latent_gain, post_attn_gain, ffn_gain, post_ffn_gain, w_query, w_query_rot, w_latent, w_key_rot, w_key_up, w_value_up, w_out, route_logits, routes, w_gate, w_up, w_down):
    batch, width = tokens.shape
    latent_size, heads, key_size = w_key_up.shape
    rot_size = w_key_rot.shape[1]
    value_size = w_value_up.shape[2]
    span = cache_latent.shape[1]
    scale = (key_size + rot_size) ** (-0.5)
    token_values = tokens.astype(jnp.float32)
    normed = rms_scale(token_values, attn_gain).astype(jnp.bfloat16)
    query_plain = jnp.dot(normed, w_query, preferred_element_type=jnp.float32).astype(jnp.bfloat16)
    query_plain = query_plain.reshape(batch, heads, key_size)
    query_rotary = jnp.dot(normed, w_query_rot, preferred_element_type=jnp.float32).astype(jnp.bfloat16)
    query_rotary = query_rotary.reshape(batch, heads, rot_size)
    latent_raw = jnp.dot(normed, w_latent, preferred_element_type=jnp.float32).astype(jnp.bfloat16)
    key_raw = jnp.dot(normed, w_key_rot, preferred_element_type=jnp.float32).astype(jnp.bfloat16)
    new_latent = rms_scale(latent_raw.astype(jnp.float32), latent_gain).astype(jnp.bfloat16)
    positions = lengths.astype(jnp.float32)
    new_rope = rotate(key_raw.astype(jnp.float32), positions).astype(jnp.bfloat16)
    query_turned = rotate(query_rotary.astype(jnp.float32), positions[:, None]).astype(jnp.bfloat16)
    query_latent = jnp.einsum('bhn,chn->bhc', query_plain.astype(jnp.float32), w_key_up.astype(jnp.float32)).astype(jnp.bfloat16)

    def attend(pieces):
        q_lat, q_turn, latents, rotary, fresh_latent, fresh_rope, length = pieces
        latents_f = latents.astype(jnp.float32)
        scores = jnp.einsum('hc,pc->hp', q_lat.astype(jnp.float32), latents_f)
        scores = (scores + jnp.einsum('hr,rp->hp', q_turn.astype(jnp.float32), rotary.astype(jnp.float32))) * scale
        self_score = (lax.optimization_barrier(jnp.sum(q_lat.astype(jnp.float32) * fresh_latent.astype(jnp.float32)[None, :], axis=-1)) + lax.optimization_barrier(jnp.sum(q_turn.astype(jnp.float32) * fresh_rope.astype(jnp.float32)[None, :], axis=-1))) * scale
        valid = jnp.arange(span, dtype=jnp.int32) < length
        masked = jnp.where(valid[None, :], scores, -jnp.inf)
        highest = jnp.maximum(lax.optimization_barrier(jnp.max(masked, axis=-1)), self_score)
        raised = jnp.exp(masked - highest[:, None])
        raised_self = jnp.exp(self_score - highest)
        total = lax.optimization_barrier(jnp.sum(raised, axis=-1)) + raised_self
        probs = (raised / total[:, None]).astype(jnp.bfloat16)
        prob_self = (raised_self / total).astype(jnp.bfloat16)
        summed = jnp.einsum('hp,pc->hc', probs.astype(jnp.float32), latents_f)
        summed = summed + prob_self.astype(jnp.float32)[:, None] * fresh_latent.astype(jnp.float32)[None, :]
        return summed.astype(jnp.bfloat16)
    head_latent = lax.map(attend, (query_latent, query_turned, cache_latent, cache_rope, new_latent, new_rope, lengths))
    values = jnp.einsum('bhc,chv->bhv', head_latent.astype(jnp.float32), w_value_up.astype(jnp.float32)).astype(jnp.bfloat16)
    flat_values = values.reshape(batch, heads * value_size)
    group_cols = heads // N_TP * value_size
    attn = jnp.zeros((batch, width), jnp.float32)
    for section in range(N_TP):
        lower = section * group_cols
        partial_sum = jnp.dot(flat_values[:, lower:lower + group_cols], w_out[lower:lower + group_cols], preferred_element_type=jnp.float32).astype(jnp.bfloat16)
        attn = attn + partial_sum.astype(jnp.float32)
    attn = attn.astype(jnp.bfloat16)
    mixed = (token_values + rms_scale(attn.astype(jnp.float32), post_attn_gain)).astype(jnp.bfloat16)
    ffn_input = rms_scale(mixed.astype(jnp.float32), ffn_gain).astype(jnp.bfloat16)
    route_weights = jax.nn.softmax(route_logits, axis=-1)
    top_k = routes.shape[1]
    experts = w_gate.shape[0]
    hidden = w_gate.shape[2]
    n_blocks = batch // GROUP
    assigned = GROUP * top_k
    flat_routes = routes.reshape(n_blocks, assigned).astype(jnp.int32)
    onehot = (flat_routes[:, :, None] == jnp.arange(experts, dtype=jnp.int32)[None, None, :]).astype(jnp.int32)
    rank = lax.optimization_barrier(jnp.sum((jnp.cumsum(onehot, axis=1) - onehot) * onehot, axis=-1)).astype(jnp.int32)
    block_ids = jnp.broadcast_to(jnp.arange(n_blocks, dtype=jnp.int32)[:, None], (n_blocks, assigned))
    token_ids = (jnp.arange(assigned, dtype=jnp.int32) // top_k).astype(jnp.int32)
    rows_in = ffn_input.reshape(n_blocks, GROUP, width)
    gathered = rows_in[:, token_ids]
    slots = jnp.zeros((n_blocks, experts, CAP, width), jnp.bfloat16).at[block_ids, flat_routes, rank].set(gathered)
    block_hidden = hidden // N_TP

    def expert(pieces):
        rows, gate_weight, up_weight, down_weight = pieces
        flat = rows.reshape(-1, width)
        gate = jnp.minimum(jnp.dot(flat, gate_weight, preferred_element_type=jnp.float32), clamp_limit)
        upward = jnp.clip(jnp.dot(flat, up_weight, preferred_element_type=jnp.float32), -clamp_limit, clamp_limit)
        active = ((upward + 1.0) * gate * jax.nn.sigmoid(sigmoid_alpha * gate)).astype(jnp.bfloat16)
        total = jnp.zeros((flat.shape[0], width), jnp.float32)
        for section in range(N_TP):
            lower = section * block_hidden
            piece = jnp.dot(active[:, lower:lower + block_hidden], down_weight[lower:lower + block_hidden], preferred_element_type=jnp.float32).astype(jnp.bfloat16)
            total = total + piece.astype(jnp.float32)
        return total.astype(jnp.bfloat16).reshape(rows.shape)
    outputs = lax.map(expert, (jnp.moveaxis(slots, 1, 0), w_gate, w_up, w_down))
    picked = outputs[flat_routes, block_ids, rank].astype(jnp.float32).reshape(batch, top_k, width)
    moe = lax.optimization_barrier(jnp.sum(picked * route_weights[:, :, None], axis=1)).astype(jnp.bfloat16)
    result = (mixed.astype(jnp.float32) + rms_scale(moe.astype(jnp.float32), post_ffn_gain)).astype(jnp.bfloat16)
    return (result, new_latent, new_rope)
```

```python
import functools

import jax
import jax.numpy as jnp
from jax import lax
from jax.experimental import pallas as pl
from jax.experimental.pallas import tpu as pltpu
from jax.sharding import PartitionSpec as P

eps_norm = 1e-06
clamp_limit = 7.0
sigmoid_alpha = 1.702
theta_base = 10000.0
MESH = pl.DeviceIdType.MESH
F32 = jnp.float32
BF16 = jnp.bfloat16


def rms_scale(values, gain):
    mean_square = jnp.mean(values * values, axis=-1, keepdims=True)
    return values * lax.rsqrt(mean_square + eps_norm) * gain


def turn(values, cosine, sine):
    half = values.shape[-1] // 2
    swapped = jnp.concatenate([values[:, half:], values[:, :half]], axis=1)
    return values * cosine + swapped * sine


def dot(a, b):
    return jnp.dot(a, b, preferred_element_type=F32)


def dot_nt(a, b):
    return lax.dot_general(a, b, (((1,), (1,)), ((), ())), preferred_element_type=F32)


def remote(src, dst, send_sem, recv_sem, where):
    return pltpu.make_async_remote_copy(
        src_ref=src,
        dst_ref=dst,
        send_sem=send_sem,
        recv_sem=recv_sem,
        device_id=where,
        device_id_type=MESH,
    )


def kernel(
    cfg,
    lengths,
    tokens,
    gains,
    latent_gain,
    cosine,
    sine,
    routes,
    routes_t,
    logits,
    cache_h,
    rope_h,
    wq_h,
    wqr_h,
    wl_h,
    wkr_h,
    wku_h,
    wvu_h,
    wo_h,
    wg_h,
    wu_h,
    wd_h,
    out_result,
    out_latent,
    out_rope,
    cache,
    rope,
    wq,
    wqr,
    wl,
    wkr,
    wku,
    wvu,
    wo,
    wg,
    wu,
    wd,
    xg,
    qsend,
    qrecv,
    qs,
    qt,
    nlat,
    nrope,
    hl,
    hsend,
    hrecv,
    asend,
    arecv,
    fg,
    sl,
    xr,
    act,
    part,
    s1,
    xsend,
    xrecv,
    rsend,
    ret,
    msend,
    mrecv,
    w_sem,
    c_sem,
    r_sem,
    tp_send,
    tp_recv,
    own_sem,
    d_send,
    d_recv,
    x_send,
    x_recv,
    sib_send,
    sib_recv,
    s1_send,
    s1_recv,
    rx_send,
    rx_recv,
    ret_send,
    ret_recv,
):
    T, EP, R, RP, LH, CP, scale = cfg
    H = T * LH
    t = lax.axis_index("tp")
    e = lax.axis_index("ep")
    C = wku.shape[0]
    KD = wq.shape[1] // LH
    RD = wkr.shape[1]
    VD = wvu.shape[1] // LH
    LC = wl.shape[1]
    D = wq.shape[0]
    Q = D // T
    G = T * RP
    S = EP * CP
    SPAN = cache.shape[1]
    sib = t + 1 - 2 * lax.rem(t, 2)

    loads = {}
    for i, (name, src, dst) in enumerate(
        [
            ("wq", wq_h, wq),
            ("wqr", wqr_h, wqr),
            ("wl", wl_h, wl),
            ("wkr", wkr_h, wkr),
            ("wku", wku_h, wku),
            ("wvu", wvu_h, wvu),
            ("wo", wo_h, wo),
            ("wg", wg_h.at[0], wg),
            ("wu", wu_h.at[0], wu),
            ("wd", wd_h.at[0], wd),
        ]
    ):
        loads[name] = pltpu.make_async_copy(src, dst, w_sem.at[i])
    for name in ("wq", "wqr", "wl", "wkr", "wku"):
        loads[name].start()

    barrier = pltpu.get_barrier_semaphore()
    for k in range(1, T):
        pl.semaphore_signal(
            barrier, inc=1, device_id={"tp": lax.rem(t + k, T)}, device_id_type=MESH
        )
    for k in range(1, EP):
        pl.semaphore_signal(
            barrier, inc=1, device_id={"ep": lax.rem(e + k, EP)}, device_id_type=MESH
        )

    def cache_copy(b):
        return pltpu.make_async_copy(cache_h.at[b], cache.at[b], c_sem.at[b])

    def rope_copy(b):
        return pltpu.make_async_copy(rope_h.at[b], rope.at[b], r_sem.at[b])

    token_values = tokens[...].astype(F32)
    xg[t] = rms_scale(token_values, gains[0:1, :]).astype(BF16)
    pl.semaphore_wait(barrier, T - 1 + EP - 1)

    def gather_tp(phase, buf):
        copies = []
        for k in range(1, T):
            c = remote(
                buf.at[t],
                buf.at[t],
                tp_send.at[phase, k],
                tp_recv.at[phase, k],
                {"tp": lax.rem(t + k, T)},
            )
            c.start()
            copies.append(c)
        return copies

    def scatter_tp(phase, src, dst):
        copies = []
        for k in range(1, T):
            peer = lax.rem(t + k, T)
            c = remote(
                src.at[peer],
                dst.at[t],
                tp_send.at[phase, k],
                tp_recv.at[phase, k],
                {"tp": peer},
            )
            c.start()
            copies.append(c)
        dst[t] = src[t]
        return copies

    def finish(copies):
        for c in copies:
            c.wait()

    copies = gather_tp(0, xg)
    for b in range(R):
        cache_copy(b).start()
        rope_copy(b).start()
    loads["wkr"].wait()
    key_raw = dot(xg[t], wkr[...]).astype(BF16).astype(F32)
    new_rope = turn(key_raw, cosine[...], sine[...]).astype(BF16)
    nrope[...] = new_rope.astype(F32)
    out_rope[...] = new_rope[:R]
    for name in ("wq", "wqr", "wl", "wku"):
        loads[name].wait()
    finish(copies)

    rows = xg[...].reshape(G, D)
    plain = dot(rows, wq[...]).astype(BF16)
    rotary = dot(rows, wqr[...]).astype(BF16)
    latent_part = dot(rows, wl[...]).astype(BF16)
    for h in range(LH):
        lat = dot_nt(plain[:, h * KD : (h + 1) * KD], wku[:, h * KD : (h + 1) * KD])
        qsend[:, :, h * C : (h + 1) * C] = lat.astype(BF16).reshape(T, RP, C)
    base = LH * C
    qsend[:, :, base : base + LH * RD] = rotary.reshape(T, RP, LH * RD)
    qsend[:, :, base + LH * RD :] = latent_part.reshape(T, RP, LC)
    copies = scatter_tp(1, qsend, qrecv)
    for name in ("wvu", "wo", "wg", "wu", "wd"):
        loads[name].start()
    ri = lax.broadcasted_iota(jnp.int32, (RP * H, RP * H), 0)
    ci = lax.broadcasted_iota(jnp.int32, (RP * H, RP * H), 1)
    head_shift = H.bit_length() - 1
    row_shift = RP.bit_length() - 1
    to_seq = (
        ci == ((ri & (H - 1)) << row_shift) + (ri >> head_shift)
    ).astype(F32).astype(BF16)
    to_head = (
        ci == ((ri & (RP - 1)) << head_shift) + (ri >> row_shift)
    ).astype(F32).astype(BF16)
    finish(copies)

    latent_raw = jnp.concatenate(
        [qrecv[s, :, base + LH * RD :] for s in range(T)], axis=1
    ).astype(F32)
    new_latent = rms_scale(latent_raw, latent_gain[...]).astype(BF16)
    out_latent[...] = new_latent[:R]
    nlat[...] = new_latent.astype(F32)
    stacked = jnp.concatenate(
        [qrecv[s, :, h * C : (h + 1) * C] for s in range(T) for h in range(LH)], axis=0
    )
    qs[...] = dot(to_seq, stacked).astype(BF16).reshape(RP, H, C)
    turned = jnp.concatenate(
        [
            turn(
                qrecv[s, :, base + h * RD : base + (h + 1) * RD].astype(F32),
                cosine[...],
                sine[...],
            ).astype(BF16)
            for s in range(T)
            for h in range(LH)
        ],
        axis=0,
    )
    qt[...] = dot(to_seq, turned).astype(BF16).reshape(RP, H, RD)
    if RP > R:
        hl[R:] = jnp.zeros((RP - R, H, C), BF16)

    def attend(b, carry):
        cache_copy(b).wait()
        rope_copy(b).wait()
        q = qs[b]
        qr = qt[b]
        latents = cache[b]
        fresh = nlat[pl.ds(b, 1), :]
        fresh_rope = nrope[pl.ds(b, 1), :]
        scores = (dot_nt(q, latents) + dot(qr, rope[b])) * scale
        own = (
            jnp.sum(q.astype(F32) * fresh, axis=1, keepdims=True)
            + jnp.sum(qr.astype(F32) * fresh_rope, axis=1, keepdims=True)
        ) * scale
        valid = lax.broadcasted_iota(jnp.int32, (H, SPAN), 1) < lengths[b]
        masked = jnp.where(valid, scores, -1e30)
        highest = jnp.maximum(jnp.max(masked, axis=1, keepdims=True), own)
        raised = jnp.where(valid, jnp.exp(masked - highest), 0.0)
        raised_own = jnp.exp(own - highest)
        total = jnp.sum(raised, axis=1, keepdims=True) + raised_own
        inverse = 1.0 / total
        probs = (raised * inverse).astype(BF16)
        prob_own = (raised_own * inverse).astype(BF16).astype(F32)
        hl[b] = (dot(probs, latents) + prob_own * fresh).astype(BF16)
        return carry

    lax.fori_loop(0, R, attend, 0)

    by_head = dot(to_head, hl[...].reshape(RP * H, C)).astype(BF16)
    hsend[...] = by_head.reshape(T, LH * RP, C)
    copies = scatter_tp(2, hsend, hrecv)
    loads["wvu"].wait()
    loads["wo"].wait()

    slot_shift = CP.bit_length() - 1
    s_lane = lax.broadcasted_iota(jnp.int32, (G, S), 1)
    e_lane = s_lane >> slot_shift
    c_lane = (s_lane & (CP - 1)).astype(F32)
    s_sub = lax.broadcasted_iota(jnp.int32, (S, G), 0)
    e_sub = s_sub >> slot_shift
    c_sub = (s_sub & (CP - 1)).astype(F32)
    gi = lax.broadcasted_iota(jnp.int32, (G, G), 0)
    gj = lax.broadcasted_iota(jnp.int32, (G, G), 1)
    lower = (gj < gi).astype(F32).astype(BF16)
    upper = (gi < gj).astype(F32).astype(BF16)
    K = routes.shape[1]
    lg = logits[...]
    lg = jnp.exp(lg - jnp.max(lg, axis=1, keepdims=True))
    weights = lg / jnp.sum(lg, axis=1, keepdims=True)
    count = jnp.zeros((G, S), F32)
    weighted = jnp.zeros((G, S), F32)
    count_t = jnp.zeros((S, G), F32)
    for k in range(K):
        hit = routes[:, k : k + 1] == e_lane
        count = jnp.where(hit, 1.0, count)
        weighted = jnp.where(hit, weights[:, k : k + 1], weighted)
        count_t = jnp.where(routes_t[k : k + 1, :] == e_sub, 1.0, count_t)
    rank = dot(lower, count.astype(BF16))
    rank_t = dot(count_t.astype(BF16), upper)
    combine = jnp.where(rank == c_lane, weighted, 0.0)
    combine_hi = combine.astype(BF16)
    combine_lo = (combine - combine_hi.astype(F32)).astype(BF16)
    dispatch = jnp.where(rank_t == c_sub, count_t, 0.0).astype(BF16)

    finish(copies)
    values = []
    for h in range(LH):
        mine = jnp.concatenate(
            [hrecv[s, h * RP : (h + 1) * RP, :] for s in range(T)], axis=0
        )
        values.append(dot(mine, wvu[:, h * VD : (h + 1) * VD]).astype(BF16))
    values = jnp.concatenate(values, axis=1)
    asend[...] = dot(values, wo[...]).astype(BF16).reshape(T, RP, D)
    finish(scatter_tp(3, asend, arecv))
    attn = arecv[0].astype(F32)
    for s in range(1, T):
        attn = attn + arecv[s].astype(F32)
    attn = attn.astype(BF16).astype(F32)
    mixed = (token_values + rms_scale(attn, gains[1:2, :])).astype(BF16).astype(F32)
    fg[t] = rms_scale(mixed, gains[2:3, :]).astype(BF16)
    finish(gather_tp(4, fg))

    mine = fg[:, :, pl.ds(pl.multiple_of(t * Q, Q), Q)].reshape(G, Q)
    sl[...] = dot(dispatch, mine).astype(BF16).reshape(EP, CP, Q)
    sent = [None]
    for k in range(1, EP):
        peer = lax.rem(e + k, EP)
        c = remote(sl.at[peer], xr.at[t, e], d_send.at[k], d_recv.at[k], {"ep": peer})
        c.start()
        sent.append(c)
    xr[t, e] = sl[e]
    pairs = T // 2
    across = []
    to_sib = []
    for k in range(EP):
        src = lax.rem(e + EP - k, EP)
        if k:
            sent[k].wait_recv()
        row = []
        for j in range(1, pairs):
            c = remote(
                xr.at[t, src],
                xr.at[t, src],
                x_send.at[k, j],
                x_recv.at[k, j],
                {"tp": lax.rem(t + 2 * j, T)},
            )
            c.start()
            row.append(c)
        across.append(row)
        c = remote(
            xr.at[t, src], xr.at[t, src], sib_send.at[k, 0], sib_recv.at[k, 0], {"tp": sib}
        )
        c.start()
        to_sib.append(c)
    for k in range(EP):
        src = lax.rem(e + EP - k, EP)
        for j in range(1, pairs):
            across[k][j - 1].wait_recv()
            quarter = lax.rem(t + T - 2 * j, T)
            c = remote(
                xr.at[quarter, src],
                xr.at[quarter, src],
                sib_send.at[k, j],
                sib_recv.at[k, j],
                {"tp": sib},
            )
            c.start()
            to_sib.append(c)
    for name in ("wg", "wu", "wd"):
        loads[name].wait()
    for c in to_sib:
        c.wait_recv()

    gate = jnp.zeros((S, wg.shape[1]), F32)
    upward = jnp.zeros((S, wg.shape[1]), F32)
    for q in range(T):
        block = xr[q].reshape(S, Q)
        gate = gate + dot(block, wg[q * Q : (q + 1) * Q, :])
        upward = upward + dot(block, wu[q * Q : (q + 1) * Q, :])
    gate = jnp.minimum(gate, clamp_limit)
    upward = jnp.clip(upward, -clamp_limit, clamp_limit)
    active = (upward + 1.0) * gate * (1.0 / (1.0 + jnp.exp(-sigmoid_alpha * gate)))
    act[...] = active.astype(BF16)

    halves = []
    for j in range(pairs - 1, -1, -1):
        quarter = lax.rem(sib + 2 * j, T)
        cols = pl.ds(pl.multiple_of(quarter * Q, Q), Q)
        part[quarter] = dot(act[...], wd[:, cols]).astype(BF16).reshape(EP, CP, Q)
        c = remote(
            part.at[quarter], s1.at[quarter], s1_send.at[j], s1_recv.at[j], {"tp": sib}
        )
        c.start()
        halves.append((j, c))
    for j in range(pairs - 1, -1, -1):
        quarter = lax.rem(t + 2 * j, T)
        cols = pl.ds(pl.multiple_of(quarter * Q, Q), Q)
        part[quarter] = dot(act[...], wd[:, cols]).astype(BF16).reshape(EP, CP, Q)
    reduced = [[None] * pairs for _ in range(EP)]
    order = list(range(1, EP)) + [0]
    for j, c in halves:
        c.wait_recv()
        if j == 0:
            continue
        quarter = lax.rem(t + 2 * j, T)
        for k in order:
            src = lax.rem(e + EP - k, EP)
            both = part[quarter, src].astype(F32) + s1[quarter, src].astype(F32)
            xsend[j, src] = both.astype(BF16)
            cc = remote(
                xsend.at[j, src],
                xrecv.at[j, src],
                rx_send.at[k, j],
                rx_recv.at[k, j],
                {"tp": quarter},
            )
            cc.start()
            reduced[k][j] = cc
    back = []
    for k in order:
        src = lax.rem(e + EP - k, EP)
        total = part[t, src].astype(F32) + s1[t, src].astype(F32)
        for j in range(1, pairs):
            reduced[k][j].wait_recv()
            total = total + xrecv[j, src].astype(F32)
        if k:
            rsend[src] = total.astype(BF16)
            c = remote(rsend.at[src], ret.at[e], ret_send.at[k], ret_recv.at[k], {"ep": src})
            c.start()
            back.append(c)
        else:
            ret[e] = total.astype(BF16)
    for c in back:
        c.wait_recv()
    returned = ret[...].reshape(S, Q)
    moe_part = dot(combine_hi, returned) + dot(combine_lo, returned)
    msend[...] = moe_part.astype(BF16).reshape(T, RP, Q)
    finish(scatter_tp(5, msend, mrecv))
    moe = jnp.concatenate([mrecv[s] for s in range(T)], axis=1).astype(F32)
    out_result[...] = (mixed + rms_scale(moe, gains[3:4, :])).astype(BF16)[:R]

    for c in sent[1:] + to_sib + [c for row in across for c in row] + back:
        c.wait_send()
    for _, c in halves:
        c.wait_send()
    for row in reduced:
        for c in row[1:]:
            c.wait_send()


def body(
    tokens,
    cache_latent,
    cache_rope,
    lengths,
    attn_gain,
    latent_gain,
    post_attn_gain,
    ffn_gain,
    post_ffn_gain,
    w_query,
    w_query_rot,
    w_latent,
    w_key_rot,
    w_key_up,
    w_value_up,
    w_out,
    route_logits,
    routes,
    w_gate,
    w_up,
    w_down,
):
    R, D = tokens.shape
    T = lax.axis_size("tp")
    EP = lax.axis_size("ep")
    C, LH, KD = w_key_up.shape
    RD = w_key_rot.shape[1]
    VD = w_value_up.shape[2]
    H = T * LH
    K = routes.shape[1]
    scale = (KD + RD) ** (-0.5)
    RP = 16
    while RP < R:
        RP *= 2
    cap = (R * T * K + EP - 1) // EP + 1
    CP = 16
    while CP < cap:
        CP *= 2
    Q = D // T
    F = w_gate.shape[2]
    LC = w_latent.shape[1]
    SPAN = cache_latent.shape[1]

    padded = jnp.pad(tokens, ((0, RP - R), (0, 0)))
    gains = jnp.stack([attn_gain, post_attn_gain, ffn_gain, post_ffn_gain]).astype(F32)
    half = RD // 2
    freqs = theta_base ** (-jnp.arange(half, dtype=F32) / half)
    angles = jnp.pad(lengths, (0, RP - R)).astype(F32)[:, None] * freqs
    cosine = jnp.cos(angles)
    sine = jnp.sin(angles)
    cosine = jnp.concatenate([cosine, cosine], axis=1)
    sine = jnp.concatenate([-sine, sine], axis=1)
    rt = jnp.pad(routes.reshape(T, R, K), ((0, 0), (0, RP - R), (0, 0)), constant_values=-1)
    rt = rt.reshape(T * RP, K)
    lg = jnp.pad(route_logits.reshape(T, R, K), ((0, 0), (0, RP - R), (0, 0)))
    lg = lg.reshape(T * RP, K)

    vm = pl.BlockSpec(memory_space=pltpu.VMEM)
    hbm = pl.BlockSpec(memory_space=pl.ANY)
    dma = pltpu.SemaphoreType.DMA
    pairs = T // 2
    QW = LH * C + LH * RD + LC

    def v(*shape, dtype=BF16):
        return pltpu.VMEM(shape, dtype)

    cfg = (T, EP, R, RP, LH, CP, scale)
    return pl.pallas_call(
        functools.partial(kernel, cfg),
        out_shape=(
            jax.ShapeDtypeStruct((R, D), BF16),
            jax.ShapeDtypeStruct((R, C), BF16),
            jax.ShapeDtypeStruct((R, RD), BF16),
        ),
        in_specs=[pl.BlockSpec(memory_space=pltpu.SMEM)] + [vm] * 8 + [hbm] * 12,
        out_specs=(vm, vm, vm),
        scratch_shapes=[
            v(R, SPAN, C),
            v(R, RD, SPAN),
            v(D, LH * KD),
            v(D, LH * RD),
            v(D, LC),
            v(D, RD),
            v(C, LH * KD),
            v(C, LH * VD),
            v(LH * VD, D),
            v(D, F),
            v(D, F),
            v(F, D),
            v(T, RP, D),
            v(T, RP, QW),
            v(T, RP, QW),
            v(RP, H, C),
            v(RP, H, RD),
            v(RP, C, dtype=F32),
            v(RP, RD, dtype=F32),
            v(RP, H, C),
            v(T, LH * RP, C),
            v(T, LH * RP, C),
            v(T, RP, D),
            v(T, RP, D),
            v(T, RP, D),
            v(EP, CP, Q),
            v(T, EP, CP, Q),
            v(EP * CP, F),
            v(T, EP, CP, Q),
            v(T, EP, CP, Q),
            v(pairs, EP, CP, Q),
            v(pairs, EP, CP, Q),
            v(EP, CP, Q),
            v(EP, CP, Q),
            v(T, RP, Q),
            v(T, RP, Q),
            dma((10,)),
            dma((R,)),
            dma((R,)),
            dma((6, T)),
            dma((6, T)),
            dma((1,)),
            dma((EP,)),
            dma((EP,)),
            dma((EP, pairs)),
            dma((EP, pairs)),
            dma((EP, pairs)),
            dma((EP, pairs)),
            dma((pairs,)),
            dma((pairs,)),
            dma((EP, pairs)),
            dma((EP, pairs)),
            dma((EP,)),
            dma((EP,)),
        ],
        compiler_params=pltpu.CompilerParams(
            collective_id=0, has_side_effects=True, vmem_limit_bytes=60 * 1024 * 1024
        ),
    )(
        lengths,
        padded,
        gains,
        latent_gain.astype(F32)[None, :],
        cosine,
        sine,
        rt,
        rt.T,
        lg,
        cache_latent,
        cache_rope,
        w_query,
        w_query_rot,
        w_latent,
        w_key_rot,
        w_key_up.reshape(C, LH * KD),
        w_value_up.reshape(C, LH * VD),
        w_out,
        w_gate,
        w_up,
        w_down,
    )


def solution(mesh):
    return jax.shard_map(
        body,
        mesh=mesh,
        in_specs=(
            P(("ep", "tp"), None),
            P(("ep", "tp"), None, None),
            P(("ep", "tp"), None, None),
            P(("ep", "tp")),
            P(),
            P(),
            P(),
            P(),
            P(),
            P(None, "tp"),
            P(None, "tp"),
            P(None, "tp"),
            P(),
            P(None, "tp", None),
            P(None, "tp", None),
            P("tp", None),
            P("ep", None),
            P("ep", None),
            P("ep", None, "tp"),
            P("ep", None, "tp"),
            P("ep", "tp", None),
        ),
        out_specs=(P(("ep", "tp"), None), P(("ep", "tp"), None), P(("ep", "tp"), None)),
        check_vma=False,
    )
```

```python
import functools

import jax
import jax.numpy as jnp
import numpy as np
from jax import lax
from jax.experimental import pallas as pl
from jax.experimental.pallas import tpu as pltpu
from jax.sharding import PartitionSpec as P

eps_norm = 1e-06
clamp_limit = 7.0
sigmoid_alpha = 1.702
theta_base = 10000.0
MESH = pl.DeviceIdType.MESH
F32 = jnp.float32
BF16 = jnp.bfloat16


def rms_scale(values, gain):
    mean_square = jnp.mean(values * values, axis=-1, keepdims=True)
    return values * lax.rsqrt(mean_square + eps_norm) * gain


def turn(values, cosine, sine):
    half = values.shape[-1] // 2
    swapped = jnp.concatenate([values[:, half:], values[:, :half]], axis=1)
    return values * cosine + swapped * sine


def dot(a, b):
    return jnp.dot(a, b, preferred_element_type=F32)


def dot_nt(a, b):
    return lax.dot_general(a, b, (((1,), (1,)), ((), ())), preferred_element_type=F32)


def remote(src, dst, send_sem, recv_sem, where):
    return pltpu.make_async_remote_copy(
        src_ref=src,
        dst_ref=dst,
        send_sem=send_sem,
        recv_sem=recv_sem,
        device_id=where,
        device_id_type=MESH,
    )


def kernel(
    cfg,
    lengths,
    tokens,
    attn_gain,
    latent_gain,
    post_attn_gain,
    ffn_gain,
    post_ffn_gain,
    routes_t,
    logits_t,
    cache_h,
    rope_h,
    wq_h,
    wqr_h,
    wl_h,
    wkr_h,
    wku_h,
    wvu_h,
    wo_h,
    wg_h,
    wu_h,
    wd_h,
    out_result,
    out_latent,
    out_rope,
    cache,
    rope,
    wq,
    wqr,
    wl,
    wkr,
    wku,
    wvu,
    wo,
    wg,
    wu,
    wd,
    xg,
    qsend,
    qrecv,
    qs,
    qt,
    nlat,
    nrope,
    hl,
    hsend,
    hrecv,
    asend,
    arecv,
    fg,
    sl,
    xr,
    act,
    part,
    s1,
    xsend,
    xrecv,
    rsend,
    ret,
    msend,
    mrecv,
    ku3,
    vu3,
    wide,
    sc,
    pb,
    w_sem,
    c_sem,
    r_sem,
    tp_send,
    tp_recv,
    own_sem,
    d_send,
    d_recv,
    x_send,
    x_recv,
    sib_send,
    sib_recv,
    s1_send,
    s1_recv,
    rx_send,
    rx_recv,
    ret_send,
    ret_recv,
):
    T, EP, R, RP, LH, CP, scale = cfg
    H = T * LH
    t = lax.axis_index("tp")
    e = lax.axis_index("ep")
    C = wku.shape[0]
    KD = wq.shape[1] // LH
    RD = wkr.shape[0]
    VD = wvu.shape[1] // LH
    LC = wl.shape[1]
    D = wq.shape[0]
    Q = D // T
    G = T * RP
    S = EP * CP
    SPAN = cache.shape[1]
    sib = t + 1 - 2 * lax.rem(t, 2)

    loads = {}
    for i, (name, src, dst) in enumerate(
        [
            ("wq", wq_h, wq),
            ("wqr", wqr_h, wqr),
            ("wl", wl_h, wl),
            ("wkr", wkr_h, wkr),
            ("wku", wku_h, ku3),
            ("wvu", wvu_h, vu3),
            ("wo", wo_h, wo),
            ("wg", wg_h.at[0], wg),
            ("wu", wu_h.at[0], wu),
            ("wd", wd_h.at[0], wd),
        ]
    ):
        loads[name] = pltpu.make_async_copy(src, dst, w_sem.at[i])
    for name in ("wku", "wkr", "wq", "wqr", "wl"):
        loads[name].start()

    barrier = pltpu.get_barrier_semaphore()
    for k in range(1, T):
        pl.semaphore_signal(
            barrier, inc=1, device_id={"tp": lax.rem(t + k, T)}, device_id_type=MESH
        )
    for k in range(1, EP):
        pl.semaphore_signal(
            barrier, inc=1, device_id={"ep": lax.rem(e + k, EP)}, device_id_type=MESH
        )

    def cache_copy(b):
        return pltpu.make_async_copy(cache_h.at[b], cache.at[b], c_sem.at[b])

    def rope_copy(b):
        return pltpu.make_async_copy(rope_h.at[b], rope.at[b], r_sem.at[b])

    def gain(ref):
        return ref[...].astype(F32)[None, :]

    def by_head_columns(source, target):
        size = source.shape[2]
        wide[...] = source[...].astype(F32).reshape(C * LH, size)
        for h in range(LH):
            target[:, h * size : (h + 1) * size] = wide[pl.ds(h, C, stride=LH), :].astype(BF16)

    token_values = jnp.concatenate(
        [tokens[...].astype(F32), jnp.zeros((RP - R, D), F32)], axis=0
    )
    xg[t] = rms_scale(token_values, gain(attn_gain)).astype(BF16)
    pl.semaphore_wait(barrier, T - 1 + EP - 1)

    def gather_tp(phase, buf):
        copies = []
        for k in range(1, T):
            c = remote(
                buf.at[t],
                buf.at[t],
                tp_send.at[phase, k],
                tp_recv.at[phase, k],
                {"tp": lax.rem(t + k, T)},
            )
            c.start()
            copies.append(c)
        return copies

    def scatter_tp(phase, src, dst):
        copies = []
        for k in range(1, T):
            peer = lax.rem(t + k, T)
            c = remote(
                src.at[peer],
                dst.at[t],
                tp_send.at[phase, k],
                tp_recv.at[phase, k],
                {"tp": peer},
            )
            c.start()
            copies.append(c)
        dst[t] = src[t]
        return copies

    def finish(copies):
        for c in copies:
            c.wait()

    copies = gather_tp(0, xg)
    for b in range(R):
        cache_copy(b).start()
        rope_copy(b).start()
    loads["wku"].wait()
    by_head_columns(ku3, wku)
    half = RD // 2
    lane = lax.broadcasted_iota(jnp.int32, (RP, RD), 1)
    row = lax.broadcasted_iota(jnp.int32, (RP, RD), 0)
    freqs = jnp.zeros((RP, RD), F32)
    for i in range(half):
        hit = (lane == i) | (lane == i + half)
        freqs = jnp.where(hit, np.float32(theta_base ** (-i / half)), freqs)
    positions = jnp.zeros((RP, RD), jnp.int32)
    for b in range(R):
        positions = jnp.where(row == b, lengths[b], positions)
    angles = positions.astype(F32) * freqs
    cosine = jnp.cos(angles)
    sine = jnp.sin(angles)
    sine = jnp.where(lane < half, -sine, sine)
    loads["wkr"].wait()
    key_raw = dot_nt(xg[t], wkr[...]).astype(BF16).astype(F32)
    new_rope = turn(key_raw, cosine, sine).astype(BF16)
    nrope[...] = new_rope.astype(F32)
    out_rope[...] = new_rope[:R]
    for name in ("wq", "wqr", "wl"):
        loads[name].wait()
    finish(copies)

    rows = xg[...].reshape(G, D)
    plain = dot(rows, wq[...]).astype(BF16)
    rotary = dot(rows, wqr[...]).astype(BF16)
    latent_part = dot(rows, wl[...]).astype(BF16)
    for h in range(LH):
        lat = dot_nt(plain[:, h * KD : (h + 1) * KD], wku[:, h * KD : (h + 1) * KD])
        qsend[:, :, h * C : (h + 1) * C] = lat.astype(BF16).reshape(T, RP, C)
    base = LH * C
    qsend[:, :, base : base + LH * RD] = rotary.reshape(T, RP, LH * RD)
    qsend[:, :, base + LH * RD :] = latent_part.reshape(T, RP, LC)
    copies = scatter_tp(1, qsend, qrecv)
    for name in ("wvu", "wo", "wg", "wu", "wd"):
        loads[name].start()
    ri = lax.broadcasted_iota(jnp.int32, (RP * H, RP * H), 0)
    ci = lax.broadcasted_iota(jnp.int32, (RP * H, RP * H), 1)
    head_shift = H.bit_length() - 1
    row_shift = RP.bit_length() - 1
    to_seq = (
        ci == ((ri & (H - 1)) << row_shift) + (ri >> head_shift)
    ).astype(F32).astype(BF16)
    to_head = (
        ci == ((ri & (RP - 1)) << head_shift) + (ri >> row_shift)
    ).astype(F32).astype(BF16)
    finish(copies)

    latent_raw = jnp.concatenate(
        [qrecv[s, :, base + LH * RD :] for s in range(T)], axis=1
    ).astype(F32)
    new_latent = rms_scale(latent_raw, gain(latent_gain)).astype(BF16)
    out_latent[...] = new_latent[:R]
    nlat[...] = new_latent.astype(F32)
    stacked = jnp.concatenate(
        [qrecv[s, :, h * C : (h + 1) * C] for s in range(T) for h in range(LH)], axis=0
    )
    qs[...] = dot(to_seq, stacked).astype(BF16).reshape(RP, H, C)
    turned = jnp.concatenate(
        [
            turn(
                qrecv[s, :, base + h * RD : base + (h + 1) * RD].astype(F32),
                cosine,
                sine,
            ).astype(BF16)
            for s in range(T)
            for h in range(LH)
        ],
        axis=0,
    )
    qt[...] = dot(to_seq, turned).astype(BF16).reshape(RP, H, RD)
    if RP > R:
        hl[R:] = jnp.zeros((RP - R, H, C), BF16)

    position = lax.broadcasted_iota(jnp.int32, (H, SPAN), 1)
    for b in range(R):
        cache_copy(b).wait()
        rope_copy(b).wait()
        scores = (dot_nt(qs[b], cache[b]) + dot(qt[b], rope[b])) * scale
        sc[b] = jnp.where(position < lengths[b], scores, -jnp.inf)
    prob_own = []
    for b in range(R):
        own = (
            jnp.sum(qs[b].astype(F32) * nlat[b : b + 1, :], axis=1, keepdims=True)
            + jnp.sum(qt[b].astype(F32) * nrope[b : b + 1, :], axis=1, keepdims=True)
        ) * scale
        masked = sc[b]
        highest = jnp.maximum(jnp.max(masked, axis=1, keepdims=True), own)
        raised = jnp.exp(masked - highest)
        raised_own = jnp.exp(own - highest)
        inverse = 1.0 / (jnp.sum(raised, axis=1, keepdims=True) + raised_own)
        pb[b] = (raised * inverse).astype(BF16)
        prob_own.append((raised_own * inverse).astype(BF16).astype(F32))
    for b in range(R):
        hl[b] = (dot(pb[b], cache[b]) + prob_own[b] * nlat[b : b + 1, :]).astype(BF16)

    by_head = dot(to_head, hl[...].reshape(RP * H, C)).astype(BF16)
    hsend[...] = by_head.reshape(T, LH * RP, C)
    copies = scatter_tp(2, hsend, hrecv)
    loads["wvu"].wait()
    by_head_columns(vu3, wvu)
    loads["wo"].wait()

    N = routes_t.shape[1]
    slot_shift = CP.bit_length() - 1
    s_sub = lax.broadcasted_iota(jnp.int32, (S, N), 0)
    e_sub = s_sub >> slot_shift
    c_sub = (s_sub & (CP - 1)).astype(F32)
    gi = lax.broadcasted_iota(jnp.int32, (N, N), 0)
    gj = lax.broadcasted_iota(jnp.int32, (N, N), 1)
    upper = (gi < gj).astype(F32).astype(BF16)
    pi = lax.broadcasted_iota(jnp.int32, (G, N), 0)
    pj = lax.broadcasted_iota(jnp.int32, (G, N), 1)
    spread = jnp.zeros((G, N), F32)
    for s in range(T):
        inside = (pj >= s * R) & (pj < (s + 1) * R)
        spread = jnp.where(inside & (pi == pj + s * (RP - R)), 1.0, spread)
    spread = spread.astype(BF16)
    lg = logits_t[...]
    lg = jnp.exp(lg - jnp.max(lg, axis=0, keepdims=True))
    weights = lg / jnp.sum(lg, axis=0, keepdims=True)
    count = jnp.zeros((S, N), F32)
    weighted = jnp.zeros((S, N), F32)
    for k in range(routes_t.shape[0]):
        hit = routes_t[k : k + 1, :] == e_sub
        count = jnp.where(hit, 1.0, count)
        weighted = jnp.where(hit, weights[k : k + 1, :], weighted)
    rank = dot(count.astype(BF16), upper)
    taken = rank == c_sub
    weighted = jnp.where(taken, weighted, 0.0)
    weighted_hi = weighted.astype(BF16)
    weighted_lo = (weighted - weighted_hi.astype(F32)).astype(BF16)
    combine_hi = dot_nt(spread, weighted_hi).astype(BF16)
    combine_lo = dot_nt(spread, weighted_lo).astype(BF16)
    dispatch = dot_nt(jnp.where(taken, count, 0.0).astype(BF16), spread).astype(BF16)

    finish(copies)
    values = []
    for h in range(LH):
        mine = jnp.concatenate(
            [hrecv[s, h * RP : (h + 1) * RP, :] for s in range(T)], axis=0
        )
        values.append(dot(mine, wvu[:, h * VD : (h + 1) * VD]).astype(BF16))
    values = jnp.concatenate(values, axis=1)
    asend[...] = dot(values, wo[...]).astype(BF16).reshape(T, RP, D)
    finish(scatter_tp(3, asend, arecv))
    attn = arecv[0].astype(F32)
    for s in range(1, T):
        attn = attn + arecv[s].astype(F32)
    attn = attn.astype(BF16).astype(F32)
    mixed = (token_values + rms_scale(attn, gain(post_attn_gain))).astype(BF16).astype(F32)
    fg[t] = rms_scale(mixed, gain(ffn_gain)).astype(BF16)
    finish(gather_tp(4, fg))

    mine = fg[:, :, pl.ds(pl.multiple_of(t * Q, Q), Q)].reshape(G, Q)
    sl[...] = dot(dispatch, mine).astype(BF16).reshape(EP, CP, Q)
    sent = [None]
    for k in range(1, EP):
        peer = lax.rem(e + k, EP)
        c = remote(sl.at[peer], xr.at[t, e], d_send.at[k], d_recv.at[k], {"ep": peer})
        c.start()
        sent.append(c)
    xr[t, e] = sl[e]
    pairs = T // 2
    across = []
    to_sib = []
    for k in range(EP):
        src = lax.rem(e + EP - k, EP)
        if k:
            sent[k].wait_recv()
        row = []
        for j in range(1, pairs):
            c = remote(
                xr.at[t, src],
                xr.at[t, src],
                x_send.at[k, j],
                x_recv.at[k, j],
                {"tp": lax.rem(t + 2 * j, T)},
            )
            c.start()
            row.append(c)
        across.append(row)
        c = remote(
            xr.at[t, src], xr.at[t, src], sib_send.at[k, 0], sib_recv.at[k, 0], {"tp": sib}
        )
        c.start()
        to_sib.append(c)
    for k in range(EP):
        src = lax.rem(e + EP - k, EP)
        for j in range(1, pairs):
            across[k][j - 1].wait_recv()
            quarter = lax.rem(t + T - 2 * j, T)
            c = remote(
                xr.at[quarter, src],
                xr.at[quarter, src],
                sib_send.at[k, j],
                sib_recv.at[k, j],
                {"tp": sib},
            )
            c.start()
            to_sib.append(c)
    for name in ("wg", "wu", "wd"):
        loads[name].wait()
    for c in to_sib:
        c.wait_recv()

    gate = jnp.zeros((S, wg.shape[1]), F32)
    upward = jnp.zeros((S, wg.shape[1]), F32)
    for q in range(T):
        block = xr[q].reshape(S, Q)
        gate = gate + dot(block, wg[q * Q : (q + 1) * Q, :])
        upward = upward + dot(block, wu[q * Q : (q + 1) * Q, :])
    gate = jnp.minimum(gate, clamp_limit)
    upward = jnp.clip(upward, -clamp_limit, clamp_limit)
    active = (upward + 1.0) * gate * (1.0 / (1.0 + jnp.exp(-sigmoid_alpha * gate)))
    act[...] = active.astype(BF16)

    halves = []
    for j in range(pairs - 1, -1, -1):
        quarter = lax.rem(sib + 2 * j, T)
        cols = pl.ds(pl.multiple_of(quarter * Q, Q), Q)
        part[quarter] = dot(act[...], wd[:, cols]).astype(BF16).reshape(EP, CP, Q)
        c = remote(
            part.at[quarter], s1.at[quarter], s1_send.at[j], s1_recv.at[j], {"tp": sib}
        )
        c.start()
        halves.append((j, c))
    for j in range(pairs - 1, -1, -1):
        quarter = lax.rem(t + 2 * j, T)
        cols = pl.ds(pl.multiple_of(quarter * Q, Q), Q)
        part[quarter] = dot(act[...], wd[:, cols]).astype(BF16).reshape(EP, CP, Q)
    reduced = [[None] * pairs for _ in range(EP)]
    order = list(range(1, EP)) + [0]
    for j, c in halves:
        c.wait_recv()
        if j == 0:
            continue
        quarter = lax.rem(t + 2 * j, T)
        for k in order:
            src = lax.rem(e + EP - k, EP)
            both = part[quarter, src].astype(F32) + s1[quarter, src].astype(F32)
            xsend[j, src] = both.astype(BF16)
            cc = remote(
                xsend.at[j, src],
                xrecv.at[j, src],
                rx_send.at[k, j],
                rx_recv.at[k, j],
                {"tp": quarter},
            )
            cc.start()
            reduced[k][j] = cc
    back = []
    for k in order:
        src = lax.rem(e + EP - k, EP)
        total = part[t, src].astype(F32) + s1[t, src].astype(F32)
        for j in range(1, pairs):
            reduced[k][j].wait_recv()
            total = total + xrecv[j, src].astype(F32)
        if k:
            rsend[src] = total.astype(BF16)
            c = remote(rsend.at[src], ret.at[e], ret_send.at[k], ret_recv.at[k], {"ep": src})
            c.start()
            back.append(c)
        else:
            ret[e] = total.astype(BF16)
    for c in back:
        c.wait_recv()
    returned = ret[...].reshape(S, Q)
    moe_part = dot(combine_hi, returned) + dot(combine_lo, returned)
    msend[...] = moe_part.astype(BF16).reshape(T, RP, Q)
    finish(scatter_tp(5, msend, mrecv))
    moe = jnp.concatenate([mrecv[s] for s in range(T)], axis=1).astype(F32)
    out_result[...] = (mixed + rms_scale(moe, gain(post_ffn_gain))).astype(BF16)[:R]

    for c in sent[1:] + to_sib + [c for row in across for c in row] + back:
        c.wait_send()
    for _, c in halves:
        c.wait_send()
    for row in reduced:
        for c in row[1:]:
            c.wait_send()


def hand_over(result, latent, rope, out_result, out_latent, out_rope):
    out_result[...] = result[...]
    out_latent[...] = latent[...]
    out_rope[...] = rope[...]


def body(
    tokens,
    cache_latent,
    cache_rope,
    lengths,
    attn_gain,
    latent_gain,
    post_attn_gain,
    ffn_gain,
    post_ffn_gain,
    w_query,
    w_query_rot,
    w_latent,
    w_key_rot,
    w_key_up,
    w_value_up,
    w_out,
    route_logits,
    routes,
    w_gate,
    w_up,
    w_down,
):
    R, D = tokens.shape
    T = lax.axis_size("tp")
    EP = lax.axis_size("ep")
    C, LH, KD = w_key_up.shape
    RD = w_key_rot.shape[1]
    VD = w_value_up.shape[2]
    H = T * LH
    K = routes.shape[1]
    scale = (KD + RD) ** (-0.5)
    RP = 16
    while RP < R:
        RP *= 2
    cap = (R * T * K + EP - 1) // EP + 1
    CP = 16
    while CP < cap:
        CP *= 2
    Q = D // T
    F = w_gate.shape[2]
    LC = w_latent.shape[1]
    SPAN = cache_latent.shape[1]

    vm = pl.BlockSpec(memory_space=pltpu.VMEM)
    hbm = pl.BlockSpec(memory_space=pl.ANY)
    dma = pltpu.SemaphoreType.DMA
    pairs = T // 2
    QW = LH * C + LH * RD + LC

    def v(*shape, dtype=BF16):
        return pltpu.VMEM(shape, dtype)

    cfg = (T, EP, R, RP, LH, CP, scale)
    outs = pl.pallas_call(
        functools.partial(kernel, cfg),
        out_shape=(
            jax.ShapeDtypeStruct((R, D), BF16),
            jax.ShapeDtypeStruct((R, C), BF16),
            jax.ShapeDtypeStruct((R, RD), BF16),
        ),
        in_specs=[pl.BlockSpec(memory_space=pltpu.SMEM)] + [vm] * 8 + [hbm] * 12,
        out_specs=(vm, vm, vm),
        scratch_shapes=[
            v(R, SPAN, C),
            v(R, RD, SPAN),
            v(D, LH * KD),
            v(D, LH * RD),
            v(D, LC),
            v(RD, D),
            v(C, LH * KD),
            v(C, LH * VD),
            v(LH * VD, D),
            v(D, F),
            v(D, F),
            v(F, D),
            v(T, RP, D),
            v(T, RP, QW),
            v(T, RP, QW),
            v(RP, H, C),
            v(RP, H, RD),
            v(RP, C, dtype=F32),
            v(RP, RD, dtype=F32),
            v(RP, H, C),
            v(T, LH * RP, C),
            v(T, LH * RP, C),
            v(T, RP, D),
            v(T, RP, D),
            v(T, RP, D),
            v(EP, CP, Q),
            v(T, EP, CP, Q),
            v(EP * CP, F),
            v(T, EP, CP, Q),
            v(T, EP, CP, Q),
            v(pairs, EP, CP, Q),
            v(pairs, EP, CP, Q),
            v(EP, CP, Q),
            v(EP, CP, Q),
            v(T, RP, Q),
            v(T, RP, Q),
            v(C, LH, KD),
            v(C, LH, VD),
            v(C * LH, KD, dtype=F32),
            v(R, H, SPAN, dtype=F32),
            v(R, H, SPAN),
            dma((10,)),
            dma((R,)),
            dma((R,)),
            dma((6, T)),
            dma((6, T)),
            dma((1,)),
            dma((EP,)),
            dma((EP,)),
            dma((EP, pairs)),
            dma((EP, pairs)),
            dma((EP, pairs)),
            dma((EP, pairs)),
            dma((pairs,)),
            dma((pairs,)),
            dma((EP, pairs)),
            dma((EP, pairs)),
            dma((EP,)),
            dma((EP,)),
        ],
        compiler_params=pltpu.CompilerParams(
            collective_id=0, has_side_effects=True, vmem_limit_bytes=60 * 1024 * 1024
        ),
    )(
        lengths,
        tokens,
        attn_gain,
        latent_gain,
        post_attn_gain,
        ffn_gain,
        post_ffn_gain,
        routes.T,
        route_logits.T,
        cache_latent,
        cache_rope,
        w_query,
        w_query_rot,
        w_latent,
        w_key_rot.T,
        w_key_up,
        w_value_up,
        w_out,
        w_gate,
        w_up,
        w_down,
    )
    return pl.pallas_call(
        hand_over,
        out_shape=tuple(jax.ShapeDtypeStruct(o.shape, o.dtype) for o in outs),
        in_specs=[vm] * 3,
        out_specs=(vm, vm, vm),
    )(*outs)


def solution(mesh):
    return jax.shard_map(
        body,
        mesh=mesh,
        in_specs=(
            P(("ep", "tp"), None),
            P(("ep", "tp"), None, None),
            P(("ep", "tp"), None, None),
            P(("ep", "tp")),
            P(),
            P(),
            P(),
            P(),
            P(),
            P(None, "tp"),
            P(None, "tp"),
            P(None, "tp"),
            P(),
            P(None, "tp", None),
            P(None, "tp", None),
            P("tp", None),
            P("ep", None),
            P("ep", None),
            P("ep", None, "tp"),
            P("ep", None, "tp"),
            P("ep", "tp", None),
        ),
        out_specs=(P(("ep", "tp"), None), P(("ep", "tp"), None), P(("ep", "tp"), None)),
        check_vma=False,
    )
```
